32 devices in a mesh: sp: 16 (over z, x, core), tp: 2 (over y).
Axes of the slice: x: 2, y: 2, z: 4, core: 2. Of those that a mesh axis runs over, the one named last changes fastest.
Arguments:
- layer_cot: bfloat16 [4096, 2048], P('sp'), may hold values from -6 to 6
- moe_input: bfloat16 [4096, 2048], P('sp'), may hold values from -6 to 6
- routes: int32 [4096, 2], P('sp'), may hold values from 0 to 15, all different within a row; in each aligned block of 256 rows (0 to 255, 256 to 511, ...) at most 48 rows name the same one
- route_weights: float32 [4096, 2], P('sp'), may hold values from 0.1 to 1.2
- gate_proj: bfloat16 [16, 2048, 1024], P('sp', None, 'tp'), may hold values from -0.125 to 0.125
- up_proj: bfloat16 [16, 2048, 1024], P('sp', None, 'tp'), may hold values from -0.125 to 0.125
- down_proj: bfloat16 [16, 1024, 2048], P('sp', 'tp'), may hold values from -0.1875 to 0.1875
- out_proj: bfloat16 [2048, 2048], P('tp'), may hold values from -0.0625 to 0.0625
- mixer_out: bfloat16 [4096, 2048], P('sp', 'tp'), may hold values from -6 to 6
- queries: bfloat16 [4096, 1024], P('sp', 'tp'), may hold values from -0.75 to 0.75
- key_rows: bfloat16 [4096, 1024], P('sp', 'tp'), may hold values from -0.75 to 0.75
- values: bfloat16 [4096, 2048], P('sp', 'tp'), may hold values from -6 to 6
- log_decay: float32 [4096, 1024], P('sp', 'tp'), may hold values from -2 to 0, as said below
- saved_state: float32 [16, 32, 32, 64], P('sp', 'tp'), may hold values from -6 to 6
Outputs:
- grad_gate: bfloat16 [16, 2048, 1024], P('sp', None, 'tp')
- grad_up: bfloat16 [16, 2048, 1024], P('sp', None, 'tp')
- grad_down: bfloat16 [16, 1024, 2048], P('sp', 'tp')
- grad_outproj: float32 [2048, 2048], P('sp', 'tp')
- grad_queries: bfloat16 [4096, 1024], P('sp', 'tp')
- grad_keys: bfloat16 [4096, 1024], P('sp', 'tp')
- grad_values: bfloat16 [4096, 2048], P('sp', 'tp')
- grad_decay: float32 [4096, 1024], P('sp', 'tp')
The draws below stay inside these ranges and needn't reach their ends.
Inputs may be any that keep to these rules, and one draw needn't show every extreme that they name: `routes`: each row names 2 different experts; no expert is named by more than 48 of the tokens of one index of sp, and in every draw some expert is named exactly 48 times by one such span. `log_decay`: log decays are negative.
All inputs are finite; a program needn't handle non-finite values.
Results may differ from the reference program's by a relative error of at most 0.014.
Values may be sent and summed in bfloat16 or wider, within the bound.
A program may use at most 192 MiB of HBM per device.

```python
import math
import jax
import jax.numpy as jnp
import numpy as np
from jax import lax

D = 2048
HEAD_COUNT = 32
KEY_CHANNELS = 32
DV = 64
FF = 1024
TOK_DEV = 256
BLOCK = 64
TOPK = 2
TOKEN_COUNT = 4096
SPANS = 16
EXPERTS = 16
CAP = 48
SLOTS = 768
HK = 1024
HV = 2048
N_TP = 2


def draw_log_decay(key, part):
    random_subkeys = jax.random.split(key, 10)
    fast_share = 0.5
    head_quick_rates = jax.random.uniform(random_subkeys[0], (HEAD_COUNT,), jnp.float32) < fast_share
    channel_fast = jnp.repeat(head_quick_rates, KEY_CHANNELS)
    slow_rates = 0.3 * 2.302585 / TOKEN_COUNT * jax.random.uniform(random_subkeys[1], (HEAD_COUNT * KEY_CHANNELS,), jnp.float32, 0.3, 1.0)
    fast_rates = jnp.exp(jax.random.uniform(random_subkeys[2], (HEAD_COUNT * KEY_CHANNELS,), jnp.float32, -4.6, -3.4))
    decay_rates = jnp.where(channel_fast, fast_rates, slow_rates)
    span_factor = jnp.exp(jax.random.uniform(random_subkeys[3], (SPANS,), jnp.float32, -0.69, 0.69))
    position_factor = jnp.repeat(span_factor, TOK_DEV)
    jitter = jnp.exp(0.5 * jnp.clip(jax.random.normal(random_subkeys[4], (TOKEN_COUNT, HEAD_COUNT * KEY_CHANNELS), jnp.float32), -2.0, 2.0) - 0.125)
    logarithm_rates = -decay_rates[None, :] * position_factor[:, None] * jitter
    spike_position = jax.random.randint(random_subkeys[5], (HEAD_COUNT, 2), 0, TOKEN_COUNT)
    spike_length = jax.random.uniform(random_subkeys[6], (HEAD_COUNT, 2), jnp.float32, -0.69, -0.22)
    token_positions = jnp.arange(TOKEN_COUNT, dtype=jnp.int32)
    spike_events = jnp.sum(jnp.where(token_positions[:, None, None] == spike_position[None, :, :], spike_length[None, :, :], 0.0), axis=2)
    spike_events = jnp.where(head_quick_rates[None, :], 0.0, spike_events)
    base_values = logarithm_rates + jnp.repeat(spike_events, KEY_CHANNELS, axis=1)
    channel_order = jax.random.permutation(random_subkeys[7], HEAD_COUNT * KEY_CHANNELS)
    strong_channel = channel_order < HEAD_COUNT * KEY_CHANNELS // 16
    run_start = jax.random.randint(random_subkeys[8], (HEAD_COUNT * KEY_CHANNELS,), 0, TOKEN_COUNT - 127)
    in_run = strong_channel[None, :] & (token_positions[:, None] >= run_start[None, :]) & (token_positions[:, None] < run_start[None, :] + 128)
    strong_values = jax.random.uniform(random_subkeys[9], (TOKEN_COUNT, HEAD_COUNT * KEY_CHANNELS), jnp.float32, -2.0, -1.6)
    return jnp.where(in_run, strong_values, base_values).astype(jnp.float32)


def raised(result, stream_key, source, target, blocks, factor):
    def block_of(axis_at):
        return (jnp.arange(result.shape[axis_at]) // (result.shape[axis_at] // blocks)).reshape((-1,) + (1,) * (result.ndim - 1 - axis_at))

    near = jax.random.permutation(stream_key, blocks)[block_of(target)]
    other_side = (block_of(target) + blocks // 2) % blocks
    return jnp.where((block_of(source) == near) | (block_of(source) == other_side), factor * result, result)


def block_scale(own_key, shape, cuts, least, high):
    def one(position, parts):
        draws = jax.random.uniform(jax.random.fold_in(jax.random.fold_in(own_key, 6), position), (parts,), jnp.float32, least / len(cuts), high / len(cuts))
        return jnp.repeat(jnp.exp(draws), shape[position] // parts).reshape((-1,) + (1,) * (len(shape) - position - 1))

    factor_of = one(*cuts[0])
    for cut in cuts[1:]:
        factor_of = factor_of * one(*cut)
    return factor_of


def routed_block(stream_key, own, number, rows, number_of, top, reach, lean):
    sequence = jax.random.permutation(stream_key, number_of)
    heavy_load, common = load_shares(number_of, rows * top, reach, lean, True), load_shares(number_of, rows * top, reach, lean, False)
    places = jnp.arange(number_of)

    def named(sizes, offset_by):
        used = int((sizes > 0).sum())
        fixed = max(1, used // 4)
        moved = fixed + (places - fixed + offset_by * (used - fixed)) % max(1, number_of - fixed)
        return jnp.zeros((number_of,), jnp.int32).at[sequence[jnp.where(places < fixed, places, moved)]].set(jnp.asarray(sizes, jnp.int32))

    sizes = jnp.where(number % 4 == 0, named(heavy_load, number // 4), named(common, number - number // 4 - 1))
    mixed = jax.random.permutation(jax.random.fold_in(own, 3), number_of)
    donor, receiver = mixed[0:number_of // 2 * 2:2], mixed[1:number_of // 2 * 2:2]
    margin = jnp.minimum(sizes[donor] - 1, reach - sizes[receiver]) // 2
    margin = jnp.where((donor == sequence[0]) | (receiver == sequence[0]) | (sizes[receiver] == 0), 0, jnp.maximum(margin, 0))
    moved = jax.random.randint(jax.random.fold_in(own, 4), (number_of // 2,), 0, 1 << 20) % (margin + 1)
    sizes = sizes.at[donor].add(-moved).at[receiver].add(moved)
    items = jnp.searchsorted(jnp.cumsum(sizes), jnp.arange(rows * top), side="right").astype(jnp.int32)
    table = items.reshape(top, rows).T
    table = table[jax.random.permutation(jax.random.fold_in(own, 1), rows)]
    offset_by = jax.random.randint(jax.random.fold_in(own, 2), (rows, 1), 0, top)
    return jnp.take_along_axis(table, (jnp.arange(top)[None, :] + offset_by) % top, axis=1)


def load_shares(number_of, total, limit, slope, full):
    loads = [(1 << 20) // math.isqrt(grade ** slope) + 1 for grade in range(1, number_of + 1)]
    largest = limit if full else min(limit, max(-(-total // number_of), total * loads[0] // sum(loads)))
    least = 1 if total - largest >= number_of - 1 else 0
    given, rest = [largest] + [least] * (number_of - 1), total - largest - least * (number_of - 1)
    while rest > 0:
        candidates = [i for i in range(1, number_of) if given[i] < largest] or [i for i in range(1, number_of) if given[i] < limit]
        whole, left = sum([loads[i] for i in candidates]), rest
        for i in candidates:
            extra = min(limit - given[i], max(1, left * loads[i] // whole), rest)
            given[i] = given[i] + extra
            rest = rest - extra
    return np.array(given)


def noise(stream_key, extent, spread, most, cuts=(), kind=jnp.bfloat16):
    gain = block_scale(stream_key, extent, cuts, -0.22, 0.18) if cuts else 1.0
    entries = jax.random.normal(stream_key, extent, jnp.float32) * spread * gain
    return jnp.minimum(jnp.maximum(entries, -most), most).astype(kind)


def bell_draw_with(stream_key, shape, width, limit, shards, heavy, held_as=jnp.bfloat16):
    entries = width * jax.random.normal(stream_key, shape, jnp.float32)
    if shards:
        entries = entries * block_scale(stream_key, shape, shards, -0.22, 0.18)
    return jnp.clip(raised(entries, jax.random.fold_in(stream_key, 3), *heavy), -limit, limit).astype(held_as)


def setup_inputs(seed: int = 0) -> dict:
    keys = jax.random.split(jax.random.key(seed), 15)
    layer_cot = bell_draw_with(keys[0], (TOKEN_COUNT, D), 1.0, 6.0, ((0, 16),), (0, 1, 16, 2.0))
    moe_input = noise(keys[1], (TOKEN_COUNT, D), 1.0, 6.0, ((0, 16),))
    routes_keys = jax.random.split(jax.random.fold_in(keys[2], 1), TOKEN_COUNT // TOK_DEV)
    routes_turns = jax.random.permutation(jax.random.fold_in(keys[2], 3), TOKEN_COUNT // TOK_DEV)
    routes = jax.vmap(lambda own, number: routed_block(jax.random.fold_in(keys[2], 2), own, number, TOK_DEV, EXPERTS, TOPK, CAP, 2))(routes_keys, routes_turns).reshape((TOKEN_COUNT, TOPK))
    route_weights = jnp.clip(0.1 + 1.1 * jax.random.uniform(keys[3], (TOKEN_COUNT, TOPK), jnp.float32) ** block_scale(keys[3], (TOKEN_COUNT, TOPK), ((0, 16),), -0.2, 0.2), 0.1, 1.2)
    gate_proj = noise(keys[4], (EXPERTS, D, FF), D ** -0.5, 0.125, ((0, 16), (2, 2)))
    up_proj = noise(keys[5], (EXPERTS, D, FF), D ** -0.5, 0.125, ((0, 16), (2, 2)))
    down_proj = noise(keys[6], (EXPERTS, FF, D), FF ** -0.5, 0.1875, ((0, 16), (1, 2)))
    out_proj = noise(keys[7], (HV, D), (4 * D) ** -0.5, 0.0625, ((0, 2),))
    mixer_out = noise(keys[8], (TOKEN_COUNT, HV), 1.0, 6.0, ((0, 16), (1, 2)))
    queries = noise(keys[9], (TOKEN_COUNT, HK), 0.125, 0.75, ((0, 16), (1, 2)))
    key_rows = noise(keys[10], (TOKEN_COUNT, HK), 0.125, 0.75, ((0, 16), (1, 2)))
    values = noise(keys[11], (TOKEN_COUNT, HV), 1.0, 6.0, ((0, 16), (1, 2)))
    log_decay = draw_log_decay(jax.random.fold_in(keys[14], 71), 0)
    saved_state = noise(keys[13], (SPANS, HEAD_COUNT, KEY_CHANNELS, DV), 1.0, 6.0, ((0, 16), (1, 2)), jnp.float32)
    return {"layer_cot": layer_cot, "moe_input": moe_input, "routes": routes, "route_weights": route_weights, "gate_proj": gate_proj, "up_proj": up_proj, "down_proj": down_proj, "out_proj": out_proj, "mixer_out": mixer_out, "queries": queries, "key_rows": key_rows, "values": values, "log_decay": log_decay, "saved_state": saved_state}


highest = lax.Precision.HIGHEST


def to_blocks(tensor, col_width):
    block_count = tensor.shape[0] // BLOCK
    head_count = tensor.shape[1] // col_width
    return tensor.astype(jnp.float32).reshape(block_count, BLOCK, head_count, col_width).transpose(0, 2, 1, 3)


def from_blocks(tensor):
    block_count, head_count, length, col_width = tensor.shape
    return tensor.transpose(0, 2, 1, 3).reshape(block_count * length, head_count * col_width)


def block_grads(queries, key_rows, values, cumulative, out_grad, state_in, from_later):
    final_log = cumulative[:, -1, :]
    token_positions = jnp.arange(cumulative.shape[1], dtype=jnp.int32)
    causal_mask = (token_positions[:, None] >= token_positions[None, :])[None, :, :, None]
    log_gaps = cumulative[:, :, None, :] - cumulative[:, None, :, :]
    decays = jnp.where(causal_mask, jnp.exp(jnp.where(causal_mask, log_gaps, 0.0)), 0.0)
    scores = jnp.einsum('htd,hsd,htsd->hts', queries, key_rows, decays, precision=highest)
    couplings = jnp.einsum('htv,hsv->hts', out_grad, values, precision=highest)
    to_end = jnp.exp(final_log[:, None, :] - cumulative)
    grad_queries = jnp.exp(cumulative) * jnp.einsum('hdv,htv->htd', state_in, out_grad, precision=highest) + jnp.einsum('hts,hsd,htsd->htd', couplings, key_rows, decays, precision=highest)
    grad_keys = to_end * jnp.einsum('hdv,hsv->hsd', from_later, values, precision=highest) + jnp.einsum('hts,htd,htsd->hsd', couplings, queries, decays, precision=highest)
    grad_values = jnp.einsum('hdv,hsd->hsv', from_later, key_rows * to_end, precision=highest) + jnp.einsum('hts,htv->hsv', scores, out_grad, precision=highest)
    grad_cumul = queries * grad_queries - key_rows * grad_keys
    to_start = jnp.exp(final_log)[:, :, None] * from_later + jnp.einsum('htd,htv->hdv', queries * jnp.exp(cumulative), out_grad, precision=highest)
    return to_start, (grad_queries, grad_keys, grad_values, grad_cumul)


def expert_grads(operands):
    rows_in, rows_cot, gate_w, up_w, down_w = operands
    pre_gate = jnp.dot(rows_in, gate_w, preferred_element_type=jnp.float32)
    pre_up = jnp.dot(rows_in, up_w, preferred_element_type=jnp.float32)
    sigmoid_gate = jax.nn.sigmoid(pre_gate)
    hidden = (pre_gate * sigmoid_gate * pre_up).astype(jnp.bfloat16)
    grad_hidden = lax.dot_general(rows_cot, down_w, (((1,), (1,)), ((), ())), preferred_element_type=jnp.float32)
    grad_down = lax.dot_general(hidden, rows_cot, (((0,), (0,)), ((), ())), preferred_element_type=jnp.float32).astype(jnp.bfloat16)
    grad_pre_gate = (grad_hidden * pre_up * sigmoid_gate * (1.0 + pre_gate * (1.0 - sigmoid_gate))).astype(jnp.bfloat16)
    grad_pre_up = (grad_hidden * pre_gate * sigmoid_gate).astype(jnp.bfloat16)
    grad_gate = lax.dot_general(rows_in, grad_pre_gate, (((0,), (0,)), ((), ())), preferred_element_type=jnp.float32).astype(jnp.bfloat16)
    grad_up = lax.dot_general(rows_in, grad_pre_up, (((0,), (0,)), ((), ())), preferred_element_type=jnp.float32).astype(jnp.bfloat16)
    group_size = FF // N_TP
    gate_parts = jnp.einsum('rjf,djf->jrd', grad_pre_gate.astype(jnp.float32).reshape(-1, N_TP, group_size), gate_w.astype(jnp.float32).reshape(D, N_TP, group_size))
    up_parts = jnp.einsum('rjf,djf->jrd', grad_pre_up.astype(jnp.float32).reshape(-1, N_TP, group_size), up_w.astype(jnp.float32).reshape(D, N_TP, group_size))
    rounded = lax.optimization_barrier((gate_parts + up_parts).astype(jnp.bfloat16))
    row_grads = jnp.sum(rounded.astype(jnp.float32), axis=0).astype(jnp.bfloat16)
    return grad_gate, grad_up, grad_down, row_grads


def mixer_grads(queries, key_rows, values, log_decay, out_grad, saved_state):
    span_blocks = TOK_DEV // BLOCK
    query_b = to_blocks(queries, KEY_CHANNELS)
    key_b = to_blocks(key_rows, KEY_CHANNELS)
    value_b = to_blocks(values, DV)
    grad_b = to_blocks(out_grad, DV)
    cumulative = jnp.cumsum(to_blocks(log_decay, KEY_CHANNELS), axis=2)
    indices = jnp.arange(query_b.shape[0], dtype=jnp.int32)

    def forward(carried, inputs):
        key_blk, value_blk, cumul_blk, block_index = inputs
        state_in = jnp.where(block_index % span_blocks == 0, saved_state[block_index // span_blocks], carried)
        final_log = cumul_blk[:, -1, :]
        state_after = jnp.exp(final_log)[:, :, None] * state_in + jnp.einsum('hsd,hsv->hdv', key_blk * jnp.exp(final_log[:, None, :] - cumul_blk), value_blk, precision=highest)
        return state_after, (state_in, state_after)

    zeros_state = jnp.zeros(saved_state.shape[1:], jnp.float32)
    _, (starts, afters) = lax.scan(forward, zeros_state, (key_b, value_b, cumulative, indices))

    def backward(carried, inputs):
        to_start, block_out = block_grads(*inputs, carried)
        return to_start, (carried,) + block_out

    _, outputs = lax.scan(backward, zeros_state, (query_b, key_b, value_b, cumulative, grad_b, starts), reverse=True)
    laters, query_grads, key_grads, value_grads, cumul_grads = outputs
    span_ends = afters[span_blocks - 1::span_blocks]
    later_ends = laters[span_blocks - 1::span_blocks]
    cross_term = jnp.sum(span_ends * later_ends, axis=3).reshape(SPANS, 1, HK)
    flat_cum = from_blocks(cumul_grads).reshape(SPANS, TOK_DEV, HK)
    reversed_sum = jnp.flip(jnp.cumsum(jnp.flip(flat_cum, 1), axis=1), 1)
    grad_decay = (reversed_sum + cross_term).reshape(TOKEN_COUNT, HK)
    return (from_blocks(query_grads).astype(jnp.bfloat16), from_blocks(key_grads).astype(jnp.bfloat16),
            from_blocks(value_grads).astype(jnp.bfloat16), grad_decay)


def reference(layer_cot, moe_input, routes, route_weights, gate_proj, up_proj, down_proj, out_proj, mixer_out, queries, key_rows, values, log_decay, saved_state):
    flat_routes = routes.reshape(-1).astype(jnp.int32)
    assign_count = flat_routes.shape[0]
    onehot = (flat_routes[:, None] == jnp.arange(EXPERTS, dtype=jnp.int32)[None, :]).astype(jnp.int32)
    per_span = onehot.reshape(SPANS, TOPK * TOK_DEV, EXPERTS)
    before = jnp.cumsum(per_span, axis=1) - per_span
    slot_ranks = jnp.sum(before * per_span, axis=2).reshape(-1)
    span_ids = jnp.arange(assign_count, dtype=jnp.int32) // (TOPK * TOK_DEV)
    places = (flat_routes * SLOTS + span_ids * CAP + slot_ranks).astype(jnp.int32)
    sources = jnp.full((EXPERTS * SLOTS,), assign_count, jnp.int32).at[places].set(jnp.arange(assign_count, dtype=jnp.int32))
    filled = sources < assign_count
    clipped = jnp.minimum(sources, assign_count - 1)
    token_ids = clipped // TOPK
    slot_weights = jnp.where(filled, route_weights.reshape(-1)[clipped], 0.0)
    expert_rows = jnp.where(filled[:, None], moe_input[token_ids], jnp.zeros((), moe_input.dtype)).reshape(EXPERTS, SLOTS, D)
    expert_cots = (slot_weights[:, None] * layer_cot[token_ids].astype(jnp.float32)).astype(jnp.bfloat16).reshape(EXPERTS, SLOTS, D)
    grad_gate, grad_up, grad_down, row_grads = lax.map(expert_grads, (expert_rows, expert_cots, gate_proj, up_proj, down_proj))
    picked = row_grads.reshape(EXPERTS * SLOTS, D)[places].astype(jnp.float32)
    moe_grad = jnp.sum(picked.reshape(TOKEN_COUNT, TOPK, D), axis=1)
    mix_grad = (layer_cot.astype(jnp.float32) + moe_grad).astype(jnp.bfloat16)
    out_grad = lax.dot_general(mix_grad, out_proj, (((1,), (1,)), ((), ())), preferred_element_type=jnp.float32).astype(jnp.bfloat16)
    grad_outproj = lax.dot_general(mix_grad, mixer_out, (((0,), (0,)), ((), ())), preferred_element_type=jnp.float32)
    grad_queries, grad_keys, grad_values, grad_decay = mixer_grads(queries, key_rows, values, log_decay, out_grad, saved_state)
    return (grad_gate, grad_up, grad_down, grad_outproj, grad_queries, grad_keys, grad_values, grad_decay)
```

```python
import functools

import jax
import jax.numpy as jnp
from jax import lax
from jax.experimental import pallas as pl
from jax.experimental.pallas import tpu as pltpu
from jax.sharding import PartitionSpec as P

KEY_CHANNELS = 32
DV = 64
BLOCK = 64
LANES = 128
GROUP = LANES // KEY_CHANNELS
GV = GROUP * DV

f32 = jnp.float32
bf16 = jnp.bfloat16


def dot(a, b, ca, cb):
    return lax.dot_general(a, b, (((ca,), (cb,)), ((), ())), preferred_element_type=f32)


def iota(shape, dim):
    return lax.broadcasted_iota(jnp.int32, shape, dim)


def state_mask():
    return (iota((GV, LANES), 0) // DV) == (iota((GV, LANES), 1) // KEY_CHANNELS)


def tile(a):
    return jnp.concatenate([a] * GROUP, axis=0)


def fold(a):
    rows = a.shape[0] // GROUP
    total = a[:rows]
    for h in range(1, GROUP):
        total = total + a[h * rows : (h + 1) * rows]
    return total


def split_dot(mask, a, parts):
    total = None
    for _ in range(parts):
        piece = a.astype(bf16)
        term = dot(mask, piece, 1, 0)
        total = term if total is None else total + term
        a = a - piece.astype(f32)
    return total


def tri(lower):
    r, c = iota((BLOCK, BLOCK), 0), iota((BLOCK, BLOCK), 1)
    return jnp.where((r >= c) if lower else (c >= r), 1.0, 0.0).astype(bf16)


def pre_kernel(k_ref, v_ref, ld_ref, s_ref, cum_ref, st_ref):
    blocks = k_ref.shape[0] // BLOCK
    mask = state_mask()
    lower = tri(True)
    state = s_ref[...]
    for n in range(blocks):
        rows = pl.ds(n * BLOCK, BLOCK)
        cum = split_dot(lower, ld_ref[rows, :], 3)
        cum_ref[rows, :] = cum
        st_ref[n] = state
        fin = cum[BLOCK - 1 : BLOCK]
        kd = (k_ref[rows, :].astype(f32) * jnp.exp(fin - cum)).astype(bf16)
        state = jnp.exp(fin) * state + fold(jnp.where(mask, dot(v_ref[rows, :], kd, 0, 0), 0.0))
    st_ref[blocks] = state


def span_kernel(q_ref, g_ref, cum_ref, t_ref):
    blocks = q_ref.shape[0] // BLOCK
    mask = state_mask()
    total = jnp.zeros((DV, LANES), f32)
    log = jnp.zeros((1, LANES), f32)
    for n in reversed(range(blocks)):
        rows = pl.ds(n * BLOCK, BLOCK)
        cum = cum_ref[rows, :]
        fin = cum[BLOCK - 1 : BLOCK]
        log = log + fin
        qd = (q_ref[rows, :].astype(f32) * jnp.exp(cum)).astype(bf16)
        total = jnp.exp(fin) * total + fold(jnp.where(mask, dot(g_ref[rows, :], qd, 0, 0), 0.0))
    t_ref[0:DV, :] = total
    t_ref[DV : DV + 8, :] = jnp.broadcast_to(jnp.exp(log), (8, LANES))


def main_kernel(
    me_ref, q_ref, k_ref, v_ref, g_ref, cum_ref, st_ref, far_ref, dq_ref, dk_ref, dv_ref, dd_ref
):
    blocks = q_ref.shape[0] // BLOCK
    spans = far_ref.shape[0]
    mask = state_mask()
    vmask = (iota((GROUP * BLOCK, GV), 0) // BLOCK) == (iota((GROUP * BLOCK, GV), 1) // DV)
    qmask = (iota((GROUP * BLOCK, LANES), 0) // BLOCK) == (
        iota((GROUP * BLOCK, LANES), 1) // KEY_CHANNELS
    )
    causal = (iota((GROUP * BLOCK, BLOCK), 0) % BLOCK) >= iota((GROUP * BLOCK, BLOCK), 1)
    upper = tri(False)
    me = me_ref[0]

    def one(i, later):
        source = spans - 1 - i
        far = far_ref[source]
        nearer = far[DV : DV + 1] * later + far[0:DV]
        return jnp.where(source > me, nearer, later)

    later = lax.fori_loop(0, spans, one, jnp.zeros((DV, LANES), f32))
    carry = jnp.sum(st_ref[blocks] * later, axis=0, keepdims=True)
    for n in reversed(range(blocks)):
        rows = pl.ds(n * BLOCK, BLOCK)
        q = q_ref[rows, :].astype(f32)
        k = k_ref[rows, :].astype(f32)
        v = v_ref[rows, :]
        g = g_ref[rows, :]
        cum = cum_ref[rows, :]
        mid = 0.5 * cum[BLOCK - 1 : BLOCK]
        half = jnp.exp(mid)
        eq = jnp.exp(cum - mid)
        ek = jnp.exp(mid - cum)
        kt = (k * ek).astype(bf16)
        qs = jnp.where(qmask, tile(q * eq), 0.0).astype(bf16)
        gs = jnp.where(vmask, tile(g.astype(f32)), 0.0).astype(bf16)
        scores = jnp.where(causal, dot(qs, kt, 1, 1), 0.0).astype(bf16)
        couple = jnp.where(causal, dot(gs, v, 1, 1), 0.0).astype(bf16)
        dq_in = fold(jnp.where(qmask, dot(couple, kt, 1, 0), 0.0))
        dk_in = dot(couple, qs, 0, 0)
        dv_in = dot(scores, gs, 0, 0)
        state = jnp.where(mask, tile(st_ref[n]), 0.0).astype(bf16)
        after = jnp.where(mask, tile(later), 0.0).astype(bf16)
        dq = eq * (dq_in + half * dot(g, state, 1, 0))
        dk = ek * (dk_in + half * dot(v, after, 1, 0))
        dv = dv_in + dot((k * (ek * half)).astype(bf16), after, 1, 1)
        dq_ref[rows, :] = dq.astype(bf16)
        dk_ref[rows, :] = dk.astype(bf16)
        dv_ref[rows, :] = dv.astype(bf16)
        suffix = split_dot(upper, q * dq - k * dk, 3) + carry
        dd_ref[rows, :] = suffix
        carry = suffix[0:1]
        qd = (q * (eq * half)).astype(bf16)
        later = half * half * later + fold(jnp.where(mask, dot(g, qd, 0, 0), 0.0))


def params(**more):
    return pltpu.CompilerParams(dimension_semantics=("arbitrary",), **more)


def cols(rows, width):
    return pl.BlockSpec((rows, width), lambda i, *_: (0, i))


def cols3(lead, rows):
    return pl.BlockSpec((lead, rows, LANES), lambda i, *_: (0, 0, i))


def mixer_pre(key_rows, values, log_decay, saved):
    tok, hk = key_rows.shape
    blocks = tok // BLOCK
    return pl.pallas_call(
        pre_kernel,
        grid=(hk // LANES,),
        in_specs=[cols(tok, LANES), cols(tok, GV), cols(tok, LANES), cols(DV, LANES)],
        out_specs=[cols(tok, LANES), cols3(blocks + 1, DV)],
        out_shape=[
            jax.ShapeDtypeStruct((tok, hk), f32),
            jax.ShapeDtypeStruct((blocks + 1, DV, hk), f32),
        ],
        compiler_params=params(),
        cost_estimate=pl.CostEstimate(flops=10**9, bytes_accessed=4 * 10**6, transcendentals=0),
        name="mixer_pre",
    )(key_rows, values, log_decay, saved)


def mixer_span(queries, out_grad, cum):
    tok, hk = queries.shape
    return pl.pallas_call(
        span_kernel,
        grid=(hk // LANES,),
        in_specs=[cols(tok, LANES), cols(tok, GV), cols(tok, LANES)],
        out_specs=cols(DV + 8, LANES),
        out_shape=jax.ShapeDtypeStruct((DV + 8, hk), f32),
        compiler_params=params(),
        cost_estimate=pl.CostEstimate(flops=10**8, bytes_accessed=2 * 10**6, transcendentals=0),
        name="mixer_span",
    )(queries, out_grad, cum)


def mixer_main(me, queries, key_rows, values, out_grad, cum, states, far):
    tok, hk = queries.shape
    hv = values.shape[1]
    blocks = tok // BLOCK
    return pl.pallas_call(
        main_kernel,
        grid_spec=pltpu.PrefetchScalarGridSpec(
            num_scalar_prefetch=1,
            grid=(hk // LANES,),
            in_specs=[
                cols(tok, LANES),
                cols(tok, LANES),
                cols(tok, GV),
                cols(tok, GV),
                cols(tok, LANES),
                cols3(blocks + 1, DV),
                cols3(far.shape[0], DV + 8),
            ],
            out_specs=[cols(tok, LANES), cols(tok, LANES), cols(tok, GV), cols(tok, LANES)],
        ),
        out_shape=[
            jax.ShapeDtypeStruct((tok, hk), bf16),
            jax.ShapeDtypeStruct((tok, hk), bf16),
            jax.ShapeDtypeStruct((tok, hv), bf16),
            jax.ShapeDtypeStruct((tok, hk), f32),
        ],
        compiler_params=params(),
        cost_estimate=pl.CostEstimate(
            flops=4 * 10**9, bytes_accessed=6 * 10**6, transcendentals=0
        ),
        name="mixer_main",
    )(me, queries, key_rows, values, out_grad, cum, states, far)


def dispatch_places(routes, experts, capacity):
    tok, top = routes.shape
    flat = routes.reshape(-1)
    count = flat.shape[0]
    onehot = flat[:, None] == jnp.arange(experts, dtype=jnp.int32)[None, :]
    earlier = jnp.arange(count)[:, None] > jnp.arange(count)[None, :]
    before = jnp.dot(
        earlier.astype(bf16), onehot.astype(bf16), preferred_element_type=f32
    )
    ranks = jnp.sum(jnp.where(onehot, before, 0.0), axis=1).astype(jnp.int32)
    return (flat * capacity + ranks).reshape(tok, top)


def body(
    layer_cot,
    moe_input,
    routes,
    route_weights,
    gate_proj,
    up_proj,
    down_proj,
    out_proj,
    mixer_out,
    queries,
    key_rows,
    values,
    log_decay,
    saved_state,
):
    sp_count = lax.axis_size("sp")
    tp_count = lax.axis_size("tp")
    local_experts = gate_proj.shape[0]
    experts = local_experts * sp_count
    tok_local, model_width = layer_cot.shape
    top_count = routes.shape[1]
    capacity = 3 * tok_local // experts
    slots = experts * capacity
    quarter = model_width // tp_count
    tp_rank = lax.axis_index("tp")

    places = dispatch_places(routes, experts, capacity)
    slot_ids = jnp.arange(slots, dtype=jnp.int32)
    hits = [slot_ids[:, None] == places[None, :, j] for j in range(top_count)]
    picks = functools.reduce(jnp.logical_or, hits).astype(bf16)
    slot_weights = sum(
        jnp.sum(jnp.where(hits[j], route_weights[None, :, j], 0.0), axis=1)
        for j in range(top_count)
    )
    part_in = lax.dynamic_slice_in_dim(moe_input, tp_rank * quarter, quarter, 1)
    part_cot = lax.dynamic_slice_in_dim(layer_cot, tp_rank * quarter, quarter, 1)
    rows_in = jnp.dot(picks, part_in, preferred_element_type=f32).astype(bf16)
    rows_cot = (
        slot_weights[:, None] * jnp.dot(picks, part_cot, preferred_element_type=f32)
    ).astype(bf16)
    rows_in = rows_in.reshape(experts, capacity, quarter)
    rows_cot = rows_cot.reshape(experts, capacity, quarter)
    got_in, got_cot = (
        lax.all_to_all(rows_in, "sp", split_axis=0, concat_axis=1, tiled=True),
        lax.all_to_all(rows_cot, "sp", split_axis=0, concat_axis=1, tiled=True),
    )
    got_in, got_cot = (
        lax.all_gather(got_in, "tp", axis=2, tiled=True),
        lax.all_gather(got_cot, "tp", axis=2, tiled=True),
    )
    saved = saved_state[0].transpose(2, 0, 1).reshape(DV, -1)
    cum, states = mixer_pre(key_rows, values, log_decay, saved)
    all_mixer = lax.all_gather(mixer_out, "sp", axis=0, tiled=True)

    pre_gate = jnp.einsum("erd,edf->erf", got_in, gate_proj, preferred_element_type=f32)
    pre_up = jnp.einsum("erd,edf->erf", got_in, up_proj, preferred_element_type=f32)
    sigmoid_gate = jax.nn.sigmoid(pre_gate)
    hidden = (pre_gate * sigmoid_gate * pre_up).astype(bf16)
    grad_hidden = jnp.einsum("erd,efd->erf", got_cot, down_proj, preferred_element_type=f32)
    grad_down = jnp.einsum("erf,erd->efd", hidden, got_cot, preferred_element_type=f32).astype(
        bf16
    )
    grad_pre_gate = (
        grad_hidden * pre_up * sigmoid_gate * (1.0 + pre_gate * (1.0 - sigmoid_gate))
    ).astype(bf16)
    grad_pre_up = (grad_hidden * pre_gate * sigmoid_gate).astype(bf16)
    grad_gate = jnp.einsum("erd,erf->edf", got_in, grad_pre_gate, preferred_element_type=f32).astype(
        bf16
    )
    grad_up = jnp.einsum("erd,erf->edf", got_in, grad_pre_up, preferred_element_type=f32).astype(
        bf16
    )
    partial_value = jnp.einsum(
        "erf,edf->erd", grad_pre_gate, gate_proj, preferred_element_type=f32
    ) + jnp.einsum("erf,edf->erd", grad_pre_up, up_proj, preferred_element_type=f32)
    summed = lax.psum_scatter(partial_value.astype(bf16), "tp", scatter_dimension=2, tiled=True)
    returned = lax.all_to_all(summed, "sp", split_axis=1, concat_axis=0, tiled=True)
    moe_grad = lax.dot_general(
        picks, returned.reshape(slots, quarter), (((0,), (0,)), ((), ())),
        preferred_element_type=f32,
    )
    mix_part = (part_cot.astype(f32) + moe_grad).astype(bf16)
    mix_grad = lax.all_gather(mix_part, "tp", axis=1, tiled=True)
    out_grad = lax.dot_general(
        mix_grad, out_proj, (((1,), (1,)), ((), ())), preferred_element_type=f32
    ).astype(bf16)
    span_part = mixer_span(queries, out_grad, cum)
    far = lax.all_gather(span_part, "sp")
    mix_cols = lax.all_to_all(mix_grad, "sp", split_axis=1, concat_axis=0, tiled=True)
    grad_outproj = lax.dot_general(
        mix_cols, all_mixer, (((0,), (0,)), ((), ())), preferred_element_type=f32
    )
    me = lax.axis_index("sp").astype(jnp.int32).reshape(1)
    grad_queries, grad_keys, grad_values, grad_decay = mixer_main(
        me, queries, key_rows, values, out_grad, cum, states, far
    )
    return (
        grad_gate,
        grad_up,
        grad_down,
        grad_outproj,
        grad_queries,
        grad_keys,
        grad_values,
        grad_decay,
    )


def solution(mesh):
    placed = (
        P("sp", None),
        P("sp", None),
        P("sp", None),
        P("sp", None),
        P("sp", None, "tp"),
        P("sp", None, "tp"),
        P("sp", "tp", None),
        P("tp", None),
        P("sp", "tp"),
        P("sp", "tp"),
        P("sp", "tp"),
        P("sp", "tp"),
        P("sp", "tp"),
        P("sp", "tp", None, None),
    )
    return jax.shard_map(
        body,
        mesh=mesh,
        in_specs=placed,
        out_specs=(
            P("sp", None, "tp"),
            P("sp", None, "tp"),
            P("sp", "tp", None),
            P("sp", "tp"),
            P("sp", "tp"),
            P("sp", "tp"),
            P("sp", "tp"),
            P("sp", "tp"),
        ),
        check_vma=False,
    )
```

```python
import functools

import jax
import jax.numpy as jnp
from jax import lax
from jax.experimental import pallas as pl
from jax.experimental.pallas import tpu as pltpu
from jax.sharding import PartitionSpec as P

KEY_CHANNELS = 32
DV = 64
BLOCK = 64
LANES = 128
GROUP = LANES // KEY_CHANNELS
GV = GROUP * DV

f32 = jnp.float32
bf16 = jnp.bfloat16


def dot(a, b, ca, cb):
    return lax.dot_general(a, b, (((ca,), (cb,)), ((), ())), preferred_element_type=f32)


def iota(shape, dim):
    return lax.broadcasted_iota(jnp.int32, shape, dim)


def state_mask():
    return (iota((GV, LANES), 0) // DV) == (iota((GV, LANES), 1) // KEY_CHANNELS)


def tile(a):
    return jnp.concatenate([a] * GROUP, axis=0)


def fold(a):
    rows = a.shape[0] // GROUP
    total = a[:rows]
    for h in range(1, GROUP):
        total = total + a[h * rows : (h + 1) * rows]
    return total


def split_dot(mask, a, parts):
    total = None
    for _ in range(parts):
        piece = a.astype(bf16)
        term = dot(mask, piece, 1, 0)
        total = term if total is None else total + term
        a = a - piece.astype(f32)
    return total


def tri(lower):
    r, c = iota((BLOCK, BLOCK), 0), iota((BLOCK, BLOCK), 1)
    return jnp.where((r >= c) if lower else (c >= r), 1.0, 0.0).astype(bf16)


def pre_kernel(k_ref, v_ref, ld_ref, s_ref, cum_ref, st_ref):
    blocks = k_ref.shape[0] // BLOCK
    mask = state_mask()
    lower = tri(True)
    state = s_ref[...]
    for n in range(blocks):
        rows = pl.ds(n * BLOCK, BLOCK)
        cum = split_dot(lower, ld_ref[rows, :], 3)
        cum_ref[rows, :] = cum
        st_ref[n] = state
        fin = cum[BLOCK - 1 : BLOCK]
        kd = (k_ref[rows, :].astype(f32) * jnp.exp(fin - cum)).astype(bf16)
        state = jnp.exp(fin) * state + fold(jnp.where(mask, dot(v_ref[rows, :], kd, 0, 0), 0.0))
    st_ref[blocks] = state


def span_kernel(q_ref, g_ref, cum_ref, t_ref):
    blocks = q_ref.shape[0] // BLOCK
    mask = state_mask()
    total = jnp.zeros((DV, LANES), f32)
    log = jnp.zeros((1, LANES), f32)
    for n in reversed(range(blocks)):
        rows = pl.ds(n * BLOCK, BLOCK)
        cum = cum_ref[rows, :]
        fin = cum[BLOCK - 1 : BLOCK]
        log = log + fin
        qd = (q_ref[rows, :].astype(f32) * jnp.exp(cum)).astype(bf16)
        total = jnp.exp(fin) * total + fold(jnp.where(mask, dot(g_ref[rows, :], qd, 0, 0), 0.0))
    t_ref[0:DV, :] = total
    t_ref[DV : DV + 8, :] = jnp.broadcast_to(jnp.exp(log), (8, LANES))


def main_kernel(
    me_ref, q_ref, k_ref, v_ref, g_ref, cum_ref, st_ref, far_ref, dq_ref, dk_ref, dv_ref, dd_ref
):
    blocks = q_ref.shape[0] // BLOCK
    spans = far_ref.shape[0]
    mask = state_mask()
    vmask = (iota((GROUP * BLOCK, GV), 0) // BLOCK) == (iota((GROUP * BLOCK, GV), 1) // DV)
    qmask = (iota((GROUP * BLOCK, LANES), 0) // BLOCK) == (
        iota((GROUP * BLOCK, LANES), 1) // KEY_CHANNELS
    )
    causal = (iota((GROUP * BLOCK, BLOCK), 0) % BLOCK) >= iota((GROUP * BLOCK, BLOCK), 1)
    upper = tri(False)
    me = me_ref[0]

    def one(i, later):
        source = spans - 1 - i
        far = far_ref[source]
        nearer = far[DV : DV + 1] * later + far[0:DV]
        return jnp.where(source > me, nearer, later)

    later = lax.fori_loop(0, spans, one, jnp.zeros((DV, LANES), f32))
    carry = jnp.sum(st_ref[blocks] * later, axis=0, keepdims=True)
    for n in reversed(range(blocks)):
        rows = pl.ds(n * BLOCK, BLOCK)
        q = q_ref[rows, :].astype(f32)
        k = k_ref[rows, :].astype(f32)
        v = v_ref[rows, :]
        g = g_ref[rows, :]
        cum = cum_ref[rows, :]
        mid = 0.5 * cum[BLOCK - 1 : BLOCK]
        half = jnp.exp(mid)
        eq = jnp.exp(cum - mid)
        ek = jnp.exp(mid - cum)
        kt = (k * ek).astype(bf16)
        qs = jnp.where(qmask, tile(q * eq), 0.0).astype(bf16)
        gs = jnp.where(vmask, tile(g.astype(f32)), 0.0).astype(bf16)
        scores = jnp.where(causal, dot(qs, kt, 1, 1), 0.0).astype(bf16)
        couple = jnp.where(causal, dot(gs, v, 1, 1), 0.0).astype(bf16)
        dq_in = fold(jnp.where(qmask, dot(couple, kt, 1, 0), 0.0))
        dk_in = dot(couple, qs, 0, 0)
        dv_in = dot(scores, gs, 0, 0)
        state = jnp.where(mask, tile(st_ref[n]), 0.0).astype(bf16)
        after = jnp.where(mask, tile(later), 0.0).astype(bf16)
        dq = eq * (dq_in + half * dot(g, state, 1, 0))
        dk = ek * (dk_in + half * dot(v, after, 1, 0))
        dv = dv_in + dot((k * (ek * half)).astype(bf16), after, 1, 1)
        dq_ref[rows, :] = dq.astype(bf16)
        dk_ref[rows, :] = dk.astype(bf16)
        dv_ref[rows, :] = dv.astype(bf16)
        suffix = split_dot(upper, q * dq - k * dk, 3) + carry
        dd_ref[rows, :] = suffix
        carry = suffix[0:1]
        qd = (q * (eq * half)).astype(bf16)
        later = half * half * later + fold(jnp.where(mask, dot(g, qd, 0, 0), 0.0))


def params(**more):
    return pltpu.CompilerParams(dimension_semantics=("arbitrary",), **more)


def cols(rows, width):
    return pl.BlockSpec((rows, width), lambda i, *_: (0, i))


def cols3(lead, rows):
    return pl.BlockSpec((lead, rows, LANES), lambda i, *_: (0, 0, i))


def mixer_pre(key_rows, values, log_decay, saved):
    tok, hk = key_rows.shape
    blocks = tok // BLOCK
    return pl.pallas_call(
        pre_kernel,
        grid=(hk // LANES,),
        in_specs=[cols(tok, LANES), cols(tok, GV), cols(tok, LANES), cols(DV, LANES)],
        out_specs=[cols(tok, LANES), cols3(blocks + 1, DV)],
        out_shape=[
            jax.ShapeDtypeStruct((tok, hk), f32),
            jax.ShapeDtypeStruct((blocks + 1, DV, hk), f32),
        ],
        compiler_params=params(),
        cost_estimate=pl.CostEstimate(flops=10**9, bytes_accessed=4 * 10**6, transcendentals=0),
        name="mixer_pre",
    )(key_rows, values, log_decay, saved)


def mixer_span(queries, out_grad, cum):
    tok, hk = queries.shape
    return pl.pallas_call(
        span_kernel,
        grid=(hk // LANES,),
        in_specs=[cols(tok, LANES), cols(tok, GV), cols(tok, LANES)],
        out_specs=cols(DV + 8, LANES),
        out_shape=jax.ShapeDtypeStruct((DV + 8, hk), f32),
        compiler_params=params(),
        cost_estimate=pl.CostEstimate(flops=10**8, bytes_accessed=2 * 10**6, transcendentals=0),
        name="mixer_span",
    )(queries, out_grad, cum)


def mixer_main(me, queries, key_rows, values, out_grad, cum, states, far):
    tok, hk = queries.shape
    hv = values.shape[1]
    blocks = tok // BLOCK
    return pl.pallas_call(
        main_kernel,
        grid_spec=pltpu.PrefetchScalarGridSpec(
            num_scalar_prefetch=1,
            grid=(hk // LANES,),
            in_specs=[
                cols(tok, LANES),
                cols(tok, LANES),
                cols(tok, GV),
                cols(tok, GV),
                cols(tok, LANES),
                cols3(blocks + 1, DV),
                cols3(far.shape[0], DV + 8),
            ],
            out_specs=[cols(tok, LANES), cols(tok, LANES), cols(tok, GV), cols(tok, LANES)],
        ),
        out_shape=[
            jax.ShapeDtypeStruct((tok, hk), bf16),
            jax.ShapeDtypeStruct((tok, hk), bf16),
            jax.ShapeDtypeStruct((tok, hv), bf16),
            jax.ShapeDtypeStruct((tok, hk), f32),
        ],
        compiler_params=params(),
        cost_estimate=pl.CostEstimate(
            flops=4 * 10**9, bytes_accessed=6 * 10**6, transcendentals=0
        ),
        name="mixer_main",
    )(me, queries, key_rows, values, out_grad, cum, states, far)


def exchange_kernel(axis, gather, count, *refs):
    ins, outs = refs[:count], refs[count : 2 * count]
    send, recv, own = refs[2 * count :]
    n = outs[0].shape[0]
    me = lax.axis_index(axis)
    barrier = pltpu.get_barrier_semaphore()

    def greet(o, _):
        pl.semaphore_signal(
            barrier, 1, device_id={axis: lax.rem(me + o, n)}, device_id_type=pl.DeviceIdType.MESH
        )
        return _

    lax.fori_loop(1, n, greet, 0)
    pl.semaphore_wait(barrier, n - 1)

    def copy(c, o):
        peer = lax.rem(me + o, n)
        return pltpu.make_async_remote_copy(
            src_ref=ins[c] if gather else ins[c].at[peer],
            dst_ref=outs[c].at[me],
            send_sem=send.at[c, o],
            recv_sem=recv.at[c, o],
            device_id={axis: peer},
            device_id_type=pl.DeviceIdType.MESH,
        )

    for c in range(count):

        def start(o, _, c=c):
            copy(c, o).start()
            return _

        lax.fori_loop(1, n, start, 0)
    locals_ = [
        pltpu.make_async_copy(ins[c] if gather else ins[c].at[me], outs[c].at[me], own.at[c])
        for c in range(count)
    ]
    for one in locals_:
        one.start()
    for one in locals_:
        one.wait()
    for c in range(count):

        def finish(o, _, c=c):
            copy(c, o).wait()
            return _

        lax.fori_loop(1, n, finish, 0)


def exchange(arrays, axis, gather, ident, name):
    n = lax.axis_size(axis)
    count = len(arrays)
    shapes = [((n,) + a.shape) if gather else a.shape for a in arrays]
    size = sum(a.size for a in arrays) * (n if gather else 1)
    return pl.pallas_call(
        functools.partial(exchange_kernel, axis, gather, count),
        in_specs=[pl.BlockSpec(memory_space=pl.ANY)] * count,
        out_specs=[pl.BlockSpec(memory_space=pl.ANY)] * count,
        out_shape=[jax.ShapeDtypeStruct(s, a.dtype) for s, a in zip(shapes, arrays)],
        scratch_shapes=[
            pltpu.SemaphoreType.DMA((count, n)),
            pltpu.SemaphoreType.DMA((count, n)),
            pltpu.SemaphoreType.DMA((count,)),
        ],
        compiler_params=pltpu.CompilerParams(collective_id=ident, has_side_effects=True),
        cost_estimate=pl.CostEstimate(
            flops=0, bytes_accessed=40 * 2 * size, transcendentals=0
        ),
        name=name,
    )(*arrays)


def dispatch_places(routes, experts, capacity):
    tok, top = routes.shape
    flat = routes.reshape(-1)
    count = flat.shape[0]
    onehot = flat[:, None] == jnp.arange(experts, dtype=jnp.int32)[None, :]
    earlier = jnp.arange(count)[:, None] > jnp.arange(count)[None, :]
    before = jnp.dot(
        earlier.astype(bf16), onehot.astype(bf16), preferred_element_type=f32
    )
    ranks = jnp.sum(jnp.where(onehot, before, 0.0), axis=1).astype(jnp.int32)
    return (flat * capacity + ranks).reshape(tok, top)


def to_expert_rows(a, local_experts, capacity):
    sources, _, width = a.shape
    return (
        a.reshape(sources, local_experts, capacity, width)
        .transpose(1, 0, 2, 3)
        .reshape(local_experts, sources * capacity, width)
    )


def body(
    layer_cot,
    moe_input,
    routes,
    route_weights,
    gate_proj,
    up_proj,
    down_proj,
    out_proj,
    mixer_out,
    queries,
    key_rows,
    values,
    log_decay,
    saved_state,
):
    sp_count = lax.axis_size("sp")
    local_experts = gate_proj.shape[0]
    experts = local_experts * sp_count
    tok_local, model_width = layer_cot.shape
    top_count = routes.shape[1]
    capacity = 3 * tok_local // experts
    slots = experts * capacity

    places = dispatch_places(routes, experts, capacity)
    slot_ids = jnp.arange(slots, dtype=jnp.int32)
    hits = [slot_ids[:, None] == places[None, :, j] for j in range(top_count)]
    picks = functools.reduce(jnp.logical_or, hits).astype(bf16)
    slot_weights = sum(
        jnp.sum(jnp.where(hits[j], route_weights[None, :, j], 0.0), axis=1)
        for j in range(top_count)
    )
    rows_in = jnp.dot(picks, moe_input, preferred_element_type=f32).astype(bf16)
    rows_cot = (
        slot_weights[:, None] * jnp.dot(picks, layer_cot, preferred_element_type=f32)
    ).astype(bf16)
    split = (experts // local_experts, local_experts * capacity, model_width)
    got = exchange([rows_in.reshape(split), rows_cot.reshape(split)], "sp", False, 0, "to_experts")
    got_in, got_cot = (to_expert_rows(a, local_experts, capacity) for a in got)
    saved = saved_state[0].transpose(2, 0, 1).reshape(DV, -1)
    cum, states = mixer_pre(key_rows, values, log_decay, saved)
    all_mixer = lax.all_gather(mixer_out, "sp", axis=0, tiled=True)

    pre_gate = jnp.einsum("erd,edf->erf", got_in, gate_proj, preferred_element_type=f32)
    pre_up = jnp.einsum("erd,edf->erf", got_in, up_proj, preferred_element_type=f32)
    sigmoid_gate = jax.nn.sigmoid(pre_gate)
    hidden = (pre_gate * sigmoid_gate * pre_up).astype(bf16)
    grad_hidden = jnp.einsum("erd,efd->erf", got_cot, down_proj, preferred_element_type=f32)
    grad_down = jnp.einsum("erf,erd->efd", hidden, got_cot, preferred_element_type=f32).astype(
        bf16
    )
    grad_pre_gate = (
        grad_hidden * pre_up * sigmoid_gate * (1.0 + pre_gate * (1.0 - sigmoid_gate))
    ).astype(bf16)
    grad_pre_up = (grad_hidden * pre_gate * sigmoid_gate).astype(bf16)
    grad_gate = jnp.einsum("erd,erf->edf", got_in, grad_pre_gate, preferred_element_type=f32).astype(
        bf16
    )
    grad_up = jnp.einsum("erd,erf->edf", got_in, grad_pre_up, preferred_element_type=f32).astype(
        bf16
    )
    partial_value = jnp.einsum(
        "erf,edf->erd", grad_pre_gate, gate_proj, preferred_element_type=f32
    ) + jnp.einsum("erf,edf->erd", grad_pre_up, up_proj, preferred_element_type=f32)
    back = (
        partial_value.astype(bf16)
        .reshape(local_experts, sp_count, capacity, model_width)
        .transpose(1, 0, 2, 3)
        .reshape(split)
    )
    back, all_mixer = lax.optimization_barrier((back, all_mixer))
    (returned,) = exchange([back], "sp", False, 1, "to_tokens")
    moe_part = lax.dot_general(
        picks, returned.reshape(slots, model_width), (((0,), (0,)), ((), ())),
        preferred_element_type=f32,
    ).astype(bf16)
    (moe_parts,) = exchange([moe_part], "tp", True, 2, "tp_parts")
    mix_grad = (layer_cot.astype(f32) + jnp.sum(moe_parts.astype(f32), axis=0)).astype(bf16)
    out_grad = lax.dot_general(
        mix_grad, out_proj, (((1,), (1,)), ((), ())), preferred_element_type=f32
    ).astype(bf16)
    span_part = mixer_span(queries, out_grad, cum)
    far = lax.all_gather(span_part, "sp")
    mix_cols = lax.all_to_all(mix_grad, "sp", split_axis=1, concat_axis=0, tiled=True)
    grad_outproj = lax.dot_general(
        mix_cols, all_mixer, (((0,), (0,)), ((), ())), preferred_element_type=f32
    )
    me = lax.axis_index("sp").astype(jnp.int32).reshape(1)
    grad_queries, grad_keys, grad_values, grad_decay = mixer_main(
        me, queries, key_rows, values, out_grad, cum, states, far
    )
    return (
        grad_gate,
        grad_up,
        grad_down,
        grad_outproj,
        grad_queries,
        grad_keys,
        grad_values,
        grad_decay,
    )


def solution(mesh):
    placed = (
        P("sp", None),
        P("sp", None),
        P("sp", None),
        P("sp", None),
        P("sp", None, "tp"),
        P("sp", None, "tp"),
        P("sp", "tp", None),
        P("tp", None),
        P("sp", "tp"),
        P("sp", "tp"),
        P("sp", "tp"),
        P("sp", "tp"),
        P("sp", "tp"),
        P("sp", "tp", None, None),
    )
    return jax.shard_map(
        body,
        mesh=mesh,
        in_specs=placed,
        out_specs=(
            P("sp", None, "tp"),
            P("sp", None, "tp"),
            P("sp", "tp", None),
            P("sp", "tp"),
            P("sp", "tp"),
            P("sp", "tp"),
            P("sp", "tp"),
            P("sp", "tp"),
        ),
        check_vma=False,
    )
```
